128 devices in a mesh: rep: 2 (over z_hi), fs: 32 (over z_lo, y, x), tp: 2 (over core).
Axes of the slice: x: 4, y: 4, z: 4 (z_hi: 2, z_lo: 2; z = z_hi * 2 + z_lo), core: 2. Of those that a mesh axis runs over, the one named last changes fastest.
Arguments:
- tokens: bfloat16 [65536, 2048], P(('rep', 'fs')), may hold values from -6 to 6
- norm_mix: bfloat16 [2048], replicated, may hold values from 0.099609375 to 1.8984375
- w_unit: bfloat16 [2048, 1024], P('fs', 'tp'), may hold values from -0.125 to 0.125
- w_value: bfloat16 [2048, 1024], P('fs', 'tp'), may hold values from -0.125 to 0.125
- spatial: bfloat16 [4, 128, 128], replicated, may hold values from -0.52734375 to 0.52734375
- spatial_bias: bfloat16 [4, 128], replicated, may hold values from 0.099609375 to 1.8984375
- group_gain: bfloat16 [1024], replicated, may hold values from 0.099609375 to 1.8984375
- group_shift: bfloat16 [1024], replicated, may hold values from -3 to 3
- w_mix_out: bfloat16 [1024, 2048], P('tp', 'fs'), may hold values from -0.1875 to 0.1875
- norm_ffn: bfloat16 [2048], replicated, may hold values from 0.099609375 to 1.8984375
- w_gate: bfloat16 [2048, 2816], P('fs', 'tp'), may hold values from -0.125 to 0.125
- w_up: bfloat16 [2048, 2816], P('fs', 'tp'), may hold values from -0.125 to 0.125
- w_down: bfloat16 [2816, 2048], P('tp', 'fs'), may hold values from -0.109375 to 0.109375
Outputs:
- layer_out: bfloat16 [65536, 2048], P(('rep', 'fs', 'tp'))
The draws below stay inside these ranges and needn't reach their ends.
All inputs are finite; a program needn't handle non-finite values.
Results may differ from the reference program's by a relative error of at most 0.008.
Values may be sent and summed in bfloat16 or wider, within the bound.
A program may use at most 128 MiB of HBM per device.

```python
import jax
import jax.numpy as jnp
from jax import lax

D = 2048
FF = 2816
GROUPS = 4
SPATIAL_WIDTH = 1024
BLOCK = 128
TOK_DEV = 1024
TOKENS = 65536


def shard_levels(key, shape, cuts, smallest, high):
    level, own = 1.0, jax.random.fold_in(key, 6)
    for dim, shards_of in cuts:
        steps = jnp.exp(jax.random.uniform(jax.random.fold_in(own, dim), (shards_of,), jnp.float32, smallest / len(cuts), high / len(cuts)))
        level = level * jnp.repeat(steps, shape[dim] // shards_of).reshape([-1 if axis == dim else 1 for axis in range(len(shape))])
    return level


def gaussian(stream_key, shape, scale, bound, split=(), held_as=jnp.bfloat16):
    values = jax.random.normal(stream_key, shape, jnp.float32) * scale
    if len(split) > 0:
        values = shard_levels(stream_key, shape, split, -0.22, 0.18) * values
    return jnp.clip(values, min=-bound, max=bound).astype(held_as)


def setup_inputs(seed: int = 0) -> dict:
    keys = jax.random.split(jax.random.key(seed), 14)
    return {
        "tokens": gaussian(keys[0], (TOKENS, D), 1.0, 6.0, ((0, 64),)),
        "norm_mix": jnp.clip(1.0 + 0.18 * jax.random.normal(keys[1], (D,), jnp.float32), 0.099609375, 1.8984375).astype(jnp.bfloat16),
        "w_unit": gaussian(keys[2], (D, SPATIAL_WIDTH), D ** -0.5, 0.125, ((0, 32), (1, 2))),
        "w_value": gaussian(keys[3], (D, SPATIAL_WIDTH), D ** -0.5, 0.125, ((0, 32), (1, 2))),
        "spatial": gaussian(keys[4], (GROUPS, BLOCK, BLOCK), (BLOCK ** -0.5), 0.52734375),
        "spatial_bias": jnp.clip(1.0 + 0.18 * jax.random.normal(keys[5], (GROUPS, BLOCK), jnp.float32), 0.099609375, 1.8984375).astype(jnp.bfloat16),
        "group_gain": jnp.clip(1.0 + 0.18 * jax.random.normal(keys[6], (SPATIAL_WIDTH,), jnp.float32), 0.099609375, 1.8984375).astype(jnp.bfloat16),
        "group_shift": gaussian(keys[7], (SPATIAL_WIDTH,), 0.5, 3.0),
        "w_mix_out": gaussian(keys[8], (SPATIAL_WIDTH, D), SPATIAL_WIDTH ** -0.5, 0.1875, ((0, 2), (1, 32))),
        "norm_ffn": jnp.clip(1.0 + 0.18 * jax.random.normal(keys[9], (D,), jnp.float32), 0.099609375, 1.8984375).astype(jnp.bfloat16),
        "w_gate": gaussian(keys[10], (D, FF), D ** -0.5, 0.125, ((0, 32), (1, 2))),
        "w_up": gaussian(keys[11], (D, FF), D ** -0.5, 0.125, ((0, 32), (1, 2))),
        "w_down": gaussian(keys[12], (FF, D), FF ** -0.5, 0.109375, ((0, 2), (1, 32))),
    }


def rms_scale(values, gain):
    values = values.astype(jnp.float32)
    scale = lax.rsqrt(lax.optimization_barrier(jnp.mean(values * values, axis=-1, keepdims=True)) + 1e-06)
    return values * scale * gain.astype(jnp.float32)

def spatial_unit(unit_pre, value_pre, spatial, spatial_bias, group_gain, group_shift):
    count, width = value_pre.shape
    groups = spatial.shape[0]
    block = spatial.shape[1]
    active = jax.nn.gelu(value_pre, approximate=True).reshape(count, groups, width // groups)
    center = lax.optimization_barrier(jnp.mean(active, axis=-1, keepdims=True))
    spread = lax.optimization_barrier(jnp.mean(jnp.square(active - center), axis=-1, keepdims=True))
    normal = ((active - center) * lax.rsqrt(spread + 1e-06)).reshape(count, width)
    normal = normal * group_gain.astype(jnp.float32) + group_shift.astype(jnp.float32)
    grouped = normal.astype(jnp.bfloat16)
    causal = jnp.tril(jnp.ones((block, block), dtype=bool))
    weights = jnp.where(causal[None], spatial, jnp.zeros_like(spatial))
    tiles = grouped.reshape(count // block, block, groups, width // groups)
    mixed = jnp.einsum('gts,nsgd->ntgd', weights.astype(jnp.float32), tiles.astype(jnp.float32))
    mixed = mixed + spatial_bias.astype(jnp.float32).T[None, :, :, None]
    return jax.nn.gelu(unit_pre, approximate=True) * mixed.reshape(count, width)

def reference(tokens, norm_mix, w_unit, w_value, spatial, spatial_bias, group_gain, group_shift, w_mix_out, norm_ffn, w_gate, w_up, w_down):

    def one_sequence(rows):
        normed = rms_scale(rows, norm_mix).astype(jnp.bfloat16)
        unit_pre = jnp.dot(normed, w_unit, preferred_element_type=jnp.float32)
        value_pre = jnp.dot(normed, w_value, preferred_element_type=jnp.float32)
        gated = spatial_unit(unit_pre, value_pre, spatial, spatial_bias, group_gain, group_shift).astype(jnp.bfloat16)
        h_mid = (rows.astype(jnp.float32) + jnp.dot(gated, w_mix_out, preferred_element_type=jnp.float32)).astype(jnp.bfloat16)
        normed_mid = rms_scale(h_mid, norm_ffn).astype(jnp.bfloat16)
        gate = jnp.dot(normed_mid, w_gate, preferred_element_type=jnp.float32)
        up = jnp.dot(normed_mid, w_up, preferred_element_type=jnp.float32)
        hidden = (jax.nn.silu(gate) * up).astype(jnp.bfloat16)
        return (h_mid.astype(jnp.float32) + jnp.dot(hidden, w_down, preferred_element_type=jnp.float32)).astype(jnp.bfloat16)
    sequences = tokens.reshape(-1, TOK_DEV, tokens.shape[1])
    return lax.map(one_sequence, sequences).reshape(tokens.shape)
```

```python
import functools

import jax
import jax.numpy as jnp
from jax import lax
from jax.experimental import pallas as pl
from jax.experimental.pallas import tpu as pltpu
from jax.sharding import PartitionSpec as P

MESH = pl.DeviceIdType.MESH
F32 = jnp.float32
BF16 = jnp.bfloat16
LANES = 128

UNIT, VALUE, MIX, PAIRS, DOWN = 0, 512, 1024, 1536, 4352
WIDTH = 5760
HALF_FF = 1408

FLOWS = (
    (0, 5, 0),
    (5, 3, 1),
    (8, 3, 0),
    (11, 1, 1),
    (12, 5, 0),
    (17, 3, 1),
    (20, 5, 0),
    (25, 3, 1),
    (28, 4, 0),
    (32, 2, 1),
    (34, 4, 0),
    (38, 2, 1),
    (40, 3, 0),
    (43, 2, 1),
)
SENDS = 14


class Flow:
    def __init__(self, index, buf, send_sems, recv_sems, where):
        first, tiles, self.order = FLOWS[index]
        self.index = index
        self.cols = pl.ds(first * LANES, tiles * LANES)
        self.buf, self.send_sems, self.recv_sems = buf, send_sems, recv_sems
        self.where = where
        self.sent = []

    def part(self, t, z, y, x, rows):
        row = {0: pl.ds(0, 64), 1: pl.ds(0, 32), 2: pl.ds(32, 32)}[rows]
        every = slice(None)
        pick = lambda i: every if i is None else i
        return self.buf.at[t, pick(z), pick(y), pick(x), row, self.cols]

    def copy(self, slot, ref, device):
        return pltpu.make_async_remote_copy(
            src_ref=ref,
            dst_ref=ref,
            send_sem=self.send_sems.at[self.index, slot],
            recv_sem=self.recv_sems.at[self.index, slot],
            device_id=device,
            device_id_type=MESH,
        )

    def send(self, slot, ref, device):
        copy = self.copy(slot, ref, device)
        copy.start()
        self.sent.append(copy)

    def arrived(self, slot, ref, device):
        self.copy(slot, ref, device).wait_recv()

    def stage(self, number):
        (self.order_xyz if self.order == 0 else self.order_zyx)(number)

    def order_xyz(self, number):
        t, z, y, x, to = self.where
        part = lambda dz, dy, dx, rows: self.part(
            t,
            lax.rem(z + dz, 2),
            None if dy is None else lax.rem(y + dy, 4),
            None if dx is None else lax.rem(x + dx, 4),
            rows,
        )
        if number == 0:
            own = part(0, 0, 0, 0)
            self.send(0, own, to["x+"])
            self.send(1, own, to["x-"])
        elif number == 1:
            self.arrived(0, part(0, 0, 3, 0), to["x-"])
            self.send(2, part(0, 0, 3, 1), to["x+"])
            self.arrived(1, part(0, 0, 1, 0), to["x+"])
            self.send(3, part(0, 0, 1, 2), to["x-"])
        elif number == 2:
            self.arrived(2, part(0, 0, 2, 1), to["x-"])
            self.arrived(3, part(0, 0, 2, 2), to["x+"])
            row = part(0, 0, None, 0)
            self.send(4, row, to["y+"])
            self.send(5, row, to["y-"])
        elif number == 3:
            self.arrived(4, part(0, 3, None, 0), to["y-"])
            self.send(6, part(0, 3, None, 1), to["y+"])
            self.arrived(5, part(0, 1, None, 0), to["y+"])
            self.send(7, part(0, 1, None, 2), to["y-"])
        elif number == 4:
            self.arrived(6, part(0, 2, None, 1), to["y-"])
            self.arrived(7, part(0, 2, None, 2), to["y+"])
            self.send(8, part(0, None, None, 1), to["z+"])
            self.send(9, part(0, None, None, 2), to["z-"])
            self.send(10, part(0, None, None, 0), to["core"])
        elif number == 5:
            self.arrived(8, part(1, None, None, 1), to["z-"])
            self.arrived(9, part(1, None, None, 2), to["z+"])
            self.send(11, part(1, None, None, 0), to["core"])
        else:
            other = 1 - t
            self.arrived(10, self.part(other, z, None, None, 0), to["core"])
            self.arrived(11, self.part(other, 1 - z, None, None, 0), to["core"])

    def order_zyx(self, number):
        t, z, y, x, to = self.where
        part = lambda dz, dy, dx, rows: self.part(
            t,
            None if dz is None else lax.rem(z + dz, 2),
            None if dy is None else lax.rem(y + dy, 4),
            lax.rem(x + dx, 4),
            rows,
        )
        if number == 0:
            self.send(0, part(0, 0, 0, 1), to["z+"])
            self.send(1, part(0, 0, 0, 2), to["z-"])
        elif number == 1:
            self.arrived(0, part(1, 0, 0, 1), to["z-"])
            self.arrived(1, part(1, 0, 0, 2), to["z+"])
            pair = part(None, 0, 0, 0)
            self.send(2, pair, to["y+"])
            self.send(3, pair, to["y-"])
        elif number == 2:
            self.arrived(2, part(None, 3, 0, 0), to["y-"])
            self.send(4, part(None, 3, 0, 1), to["y+"])
            self.arrived(3, part(None, 1, 0, 0), to["y+"])
            self.send(5, part(None, 1, 0, 2), to["y-"])
        elif number == 3:
            self.arrived(4, part(None, 2, 0, 1), to["y-"])
            self.arrived(5, part(None, 2, 0, 2), to["y+"])
            line = part(None, None, 0, 0)
            self.send(6, line, to["x+"])
            self.send(7, line, to["x-"])
            self.send(10, line, to["core"])
        elif number == 4:
            self.arrived(6, part(None, None, 3, 0), to["x-"])
            self.send(8, part(None, None, 3, 1), to["x+"])
            self.arrived(7, part(None, None, 1, 0), to["x+"])
            self.send(9, part(None, None, 1, 2), to["x-"])
            self.send(11, part(None, None, 3, 0), to["core"])
            self.send(12, part(None, None, 1, 0), to["core"])
        elif number == 5:
            self.arrived(8, part(None, None, 2, 1), to["x-"])
            self.arrived(9, part(None, None, 2, 2), to["x+"])
            self.send(13, part(None, None, 2, 0), to["core"])
        else:
            other = 1 - t
            for slot, dx in ((10, 0), (11, 3), (12, 1), (13, 2)):
                place = lax.rem(x + dx, 4)
                self.arrived(slot, self.part(other, None, None, place, 0), to["core"])


def rms_rows(source, gain, target, rows):
    values = source[rows, :].astype(F32)
    scale = lax.rsqrt(jnp.mean(values * values, axis=-1, keepdims=True) + 1e-06)
    target[rows, :] = (values * scale * gain[...].astype(F32)).astype(BF16)


def dot(a, b):
    return jnp.dot(a, b, preferred_element_type=F32)


def dot_nt(a, b):
    return lax.dot_general(a, b, (((1,), (1,)), ((), ())), preferred_element_type=F32)


def kernel(
    tokens,
    shard,
    norm_mix,
    spatial,
    bias,
    gain,
    shift,
    norm_ffn,
    out,
    buf,
    rows_in,
    normed,
    pre,
    gated,
    hmid,
    hidden,
    staged,
    send_sems,
    recv_sems,
    local_sems,
    out_sems,
):
    r, f, t = lax.axis_index("rep"), lax.axis_index("fs"), lax.axis_index("tp")
    z, y, x = f // 16, lax.rem(f // 4, 4), lax.rem(f, 4)
    up, down = lax.rem(2 * r + z + 1, 4), lax.rem(2 * r + z + 3, 4)
    at = lambda zz, yy, xx, tt: (zz // 2, lax.rem(zz, 2) * 16 + yy * 4 + xx, tt)
    here = 2 * r + z
    to = {
        "x+": at(here, y, lax.rem(x + 1, 4), t),
        "x-": at(here, y, lax.rem(x + 3, 4), t),
        "y+": at(here, lax.rem(y + 1, 4), x, t),
        "y-": at(here, lax.rem(y + 3, 4), x, t),
        "z+": at(up, y, x, t),
        "z-": at(down, y, x, t),
        "core": at(here, y, x, 1 - t),
    }

    own = pltpu.make_async_copy(shard, buf.at[t, z, y, x], local_sems.at[0])
    own.start()
    count = rows_in.shape[0]
    load = pltpu.make_async_copy(
        tokens.at[pl.ds(t * count, count)], rows_in, local_sems.at[1]
    )
    load.start()

    barrier = pltpu.get_barrier_semaphore()
    for device in to.values():
        pl.semaphore_signal(barrier, inc=1, device_id=device, device_id_type=MESH)
    pl.semaphore_wait(barrier, len(to))
    own.wait()

    where = (t, z, y, x, to)
    flows = [Flow(i, buf, send_sems, recv_sems, where) for i in range(len(FLOWS))]
    for flow in flows:
        flow.stage(0)
    load.wait()

    blocks = count // LANES

    def over_rows(body):
        def step(i, carry):
            body(pl.ds(pl.multiple_of(i * LANES, LANES), LANES))
            return carry

        lax.fori_loop(0, blocks, step, 0)

    def columns(tt, first, size):
        return buf[tt, :, :, :, :, pl.ds(first, size)].reshape(2048, size)

    def spatial_group(g):
        tt, low = g // 2, (g % 2) * 256
        pre[:, 0:256] = dot(normed[...], columns(tt, UNIT + low, 256))
        pre[:, 256:512] = dot(normed[...], columns(tt, VALUE + low, 256))
        at_row = lax.broadcasted_iota(jnp.int32, (128, 128), 0)
        at_col = lax.broadcasted_iota(jnp.int32, (128, 128), 1)
        weights = jnp.where(at_row >= at_col, spatial[g], jnp.zeros((128, 128), BF16))
        g_gain = gain[:, g * 256 : g * 256 + 256].astype(F32)
        g_shift = shift[:, g * 256 : g * 256 + 256].astype(F32)

        def body(rows):
            active = jax.nn.gelu(pre[rows, 256:512], approximate=True)
            center = jnp.mean(active, axis=-1, keepdims=True)
            off = active - center
            spread = jnp.mean(off * off, axis=-1, keepdims=True)
            grouped = off * lax.rsqrt(spread + 1e-06) * g_gain + g_shift
            mixed = dot(weights, grouped.astype(BF16)) + bias[g]
            value = jax.nn.gelu(pre[rows, 0:256], approximate=True) * mixed
            gated[rows, g * 256 : g * 256 + 256] = value.astype(BF16)

        over_rows(body)

    def mix_out(block, carry):
        zz, yy = block // 4, lax.rem(block, 4)
        cols = pl.ds(pl.multiple_of(block * 256, 256), 256)
        total = rows_in[:, cols].astype(F32)
        for tt in range(2):
            w = buf[tt, zz, yy, :, :, pl.ds(MIX, 512)].reshape(256, 512)
            total = total + dot_nt(gated[:, tt * 512 : tt * 512 + 512], w)
        hmid[:, cols] = total.astype(BF16)
        return carry

    def gate_up(tt):
        def step(i, carry):
            first = pl.multiple_of(PAIRS + i * 256, 256)
            both = dot(normed[...], columns(tt, first, 256))
            value = jax.nn.silu(both[:, 0:128]) * both[:, 128:256]
            into = pl.ds(pl.multiple_of(tt * HALF_FF + i * 128, 128), 128)
            hidden[:, into] = value.astype(BF16)
            return carry

        return step

    def out_copy(block, slot):
        cols = pl.ds(pl.multiple_of(block * 256, 256), 256)
        return pltpu.make_async_copy(
            staged.at[slot], out.at[:, cols], out_sems.at[slot]
        )

    def project_down(block, carry):
        zz, yy = block // 4, lax.rem(block, 4)
        cols = pl.ds(pl.multiple_of(block * 256, 256), 256)
        total = hmid[:, cols].astype(F32)
        for tt in range(2):
            w = buf[tt, zz, yy, :, :, pl.ds(DOWN, HALF_FF)].reshape(256, HALF_FF)
            total = total + dot_nt(hidden[:, tt * HALF_FF : tt * HALF_FF + HALF_FF], w)
        staged[block] = total.astype(BF16)
        out_copy(block, block).start()
        return carry

    over_rows(functools.partial(rms_rows, rows_in, norm_mix, normed))
    for number in range(1, 7):
        for flow in flows:
            flow.stage(number)
    for g in range(4):
        spatial_group(g)
    lax.fori_loop(0, 8, mix_out, 0)
    over_rows(functools.partial(rms_rows, hmid, norm_ffn, normed))
    for tt in range(2):
        lax.fori_loop(0, 11, gate_up(tt), 0)
    lax.fori_loop(0, 8, project_down, 0)
    for block in range(8):
        out_copy(block, block).wait()
    for flow in flows:
        for copy in flow.sent:
            copy.wait_send()


def on_device(
    tokens,
    norm_mix,
    w_unit,
    w_value,
    spatial,
    spatial_bias,
    group_gain,
    group_shift,
    w_mix_out,
    norm_ffn,
    w_gate,
    w_up,
    w_down,
):
    count, width = tokens.shape
    half = count // 2
    pairs = jnp.stack([w_gate.reshape(64, 11, 128), w_up.reshape(64, 11, 128)], axis=2)
    shard = jnp.concatenate(
        [w_unit, w_value, w_mix_out.T, pairs.reshape(64, 2816), w_down.T], axis=1
    )
    any_space = pl.BlockSpec(memory_space=pl.ANY)
    vmem = pl.BlockSpec(memory_space=pltpu.VMEM)
    return pl.pallas_call(
        kernel,
        out_shape=jax.ShapeDtypeStruct((half, width), BF16),
        in_specs=[any_space, any_space] + [vmem] * 6,
        out_specs=any_space,
        scratch_shapes=[
            pltpu.VMEM((2, 2, 4, 4, 64, WIDTH), BF16),
            pltpu.VMEM((half, width), BF16),
            pltpu.VMEM((half, width), BF16),
            pltpu.VMEM((half, 512), F32),
            pltpu.VMEM((half, 1024), BF16),
            pltpu.VMEM((half, width), BF16),
            pltpu.VMEM((half, 2 * HALF_FF), BF16),
            pltpu.VMEM((8, half, 256), BF16),
            pltpu.SemaphoreType.DMA((len(FLOWS), SENDS)),
            pltpu.SemaphoreType.DMA((len(FLOWS), SENDS)),
            pltpu.SemaphoreType.DMA((2,)),
            pltpu.SemaphoreType.DMA((8,)),
        ],
        compiler_params=pltpu.CompilerParams(
            collective_id=0, has_side_effects=True, vmem_limit_bytes=67043328
        ),
    )(
        tokens,
        shard,
        norm_mix.reshape(1, -1),
        spatial,
        spatial_bias.astype(F32)[:, :, None],
        group_gain.reshape(1, -1),
        group_shift.reshape(1, -1),
        norm_ffn.reshape(1, -1),
    )


def solution(mesh):
    placed = (
        P(("rep", "fs"), None),
        P(),
        P("fs", "tp"),
        P("fs", "tp"),
        P(),
        P(),
        P(),
        P(),
        P("tp", "fs"),
        P(),
        P("fs", "tp"),
        P("fs", "tp"),
        P("tp", "fs"),
    )
    return jax.shard_map(
        on_device,
        mesh=mesh,
        in_specs=placed,
        out_specs=P(("rep", "fs", "tp"), None),
        check_vma=False,
    )
```

```python
import functools

import jax
import jax.numpy as jnp
from jax import lax
from jax.experimental import pallas as pl
from jax.experimental.pallas import tpu as pltpu
from jax.sharding import PartitionSpec as P

MESH = pl.DeviceIdType.MESH
F32 = jnp.float32
BF16 = jnp.bfloat16
LANES = 128

UNIT, VALUE, MIX, PAIRS, DOWN = 0, 512, 1024, 1536, 4352
WIDTH = 5760
HALF_FF = 1408

FLOWS = (
    (0, 3, "xyz"),
    (3, 3, "xzy"),
    (6, 2, "xyz"),
    (8, 2, "yxz"),
    (10, 2, "yzx"),
    (12, 4, "zyx"),
    (16, 4, "yxz"),
    (20, 4, "xyz"),
    (24, 4, "yzx"),
    (28, 3, "yxz"),
    (31, 3, "yxz"),
    (34, 3, "xzy"),
    (37, 2, "xzy"),
    (39, 2, "xzy"),
    (41, 2, "zyx"),
    (43, 2, "xyz"),
)
DOWN_PARTS = (
    (0, 896),
    (896, 512),
)
SCHEDULE = (
    ("s", 0, 0),
    ("s", 3, 0),
    ("s", 10, 0),
    ("n1",),
    ("s", 2, 0),
    ("s", 1, 0),
    ("s", 8, 0),
    ("s", 3, 1),
    ("s", 0, 1),
    ("s", 7, 0),
    ("s", 10, 1),
    ("s", 2, 1),
    ("s", 4, 0),
    ("s", 1, 1),
    ("s", 8, 1),
    ("s", 3, 2),
    ("s", 0, 2),
    ("s", 11, 0),
    ("s", 10, 2),
    ("s", 7, 1),
    ("s", 4, 1),
    ("s", 2, 2),
    ("s", 1, 2),
    ("s", 8, 2),
    ("s", 3, 3),
    ("s", 12, 0),
    ("s", 11, 1),
    ("s", 0, 3),
    ("s", 1, 3),
    ("s", 4, 2),
    ("s", 6, 0),
    ("s", 8, 3),
    ("s", 2, 3),
    ("s", 10, 3),
    ("s", 7, 2),
    ("s", 13, 0),
    ("s", 4, 3),
    ("s", 0, 4),
    ("s", 3, 4),
    ("s", 9, 0),
    ("s", 5, 0),
    ("s", 12, 1),
    ("s", 11, 2),
    ("s", 1, 4),
    ("s", 6, 1),
    ("s", 0, 5),
    ("s", 2, 4),
    ("s", 8, 4),
    ("s", 10, 4),
    ("s", 0, 6),
    ("s", 13, 1),
    ("s", 3, 5),
    ("s", 7, 3),
    ("s", 5, 1),
    ("s", 9, 1),
    ("s", 11, 3),
    ("s", 4, 4),
    ("s", 12, 2),
    ("s", 1, 5),
    ("s", 6, 2),
    ("s", 3, 6),
    ("s", 2, 5),
    ("s", 7, 4),
    ("s", 14, 0),
    ("s", 8, 5),
    ("s", 13, 2),
    ("s", 5, 2),
    ("s", 9, 2),
    ("s", 1, 6),
    ("g", 0),
    ("s", 2, 6),
    ("s", 4, 5),
    ("g", 1),
    ("s", 10, 5),
    ("s", 12, 3),
    ("g", 2),
    ("s", 6, 3),
    ("s", 8, 6),
    ("s", 11, 4),
    ("s", 4, 6),
    ("s", 15, 0),
    ("g", 3),
    ("s", 5, 3),
    ("s", 10, 6),
    ("s", 9, 3),
    ("m", 0, 4),
    ("s", 6, 4),
    ("m", 4, 6),
    ("s", 12, 4),
    ("s", 15, 1),
    ("m", 6, 8),
    ("n2",),
    ("s", 14, 1),
    ("s", 7, 5),
    ("u", 0, 4, 2),
    ("s", 13, 3),
    ("s", 11, 5),
    ("u", 0, 6, 2),
    ("u", 1, 6, 2),
    ("s", 12, 5),
    ("s", 14, 2),
    ("s", 7, 6),
    ("u", 1, 4, 2),
    ("s", 5, 4),
    ("s", 11, 6),
    ("s", 12, 6),
    ("s", 9, 4),
    ("s", 15, 2),
    ("s", 13, 4),
    ("s", 6, 5),
    ("s", 14, 3),
    ("u", 0, 2, 2),
    ("s", 15, 3),
    ("s", 5, 5),
    ("u", 0, 0, 2),
    ("s", 13, 5),
    ("s", 15, 4),
    ("s", 6, 6),
    ("u", 1, 2, 2),
    ("s", 14, 4),
    ("s", 9, 5),
    ("u", 0, 8, 3),
    ("s", 5, 6),
    ("s", 13, 6),
    ("u", 1, 0, 2),
    ("d", 0, 0, 4),
    ("s", 14, 5),
    ("s", 15, 5),
    ("d", 0, 4, 6),
    ("s", 9, 6),
    ("u", 1, 8, 3),
    ("s", 14, 6),
    ("d", 0, 6, 8),
    ("s", 15, 6),
    ("d", 1, 0, 8),
)
SENDS = 14


class Flow:
    def __init__(self, index, buf, send_sems, recv_sems, where):
        first, tiles, order = FLOWS[index]
        self.index = index
        self.cols = pl.ds(first * LANES, tiles * LANES)
        self.buf, self.send_sems, self.recv_sems = buf, send_sems, recv_sems
        self.core, self.home, self.to = where
        self.sent = []
        self.stages = self.plan(order)

    def part(self, place, rows, core):
        row = (pl.ds(0, 64), pl.ds(0, 32), pl.ds(32, 32))[rows]
        at = [slice(None) if place[a] is None else place[a] for a in "zyx"]
        return self.buf.at[core, at[0], at[1], at[2], row, self.cols]

    def copy(self, slot, ref, device):
        return pltpu.make_async_remote_copy(
            src_ref=ref,
            dst_ref=ref,
            send_sem=self.send_sems.at[self.index, slot],
            recv_sem=self.recv_sems.at[self.index, slot],
            device_id=self.to[device],
            device_id_type=MESH,
        )

    def send(self, slot, place, rows, device):
        copy = self.copy(slot, self.part(place, rows, self.core), device)
        copy.start()
        self.sent.append(copy)

    def arrived(self, slot, place, rows, device):
        core = 1 - self.core if device == "core" else self.core
        self.copy(slot, self.part(place, rows, core), device).wait_recv()

    def stage(self, number):
        for action, args in self.stages[number]:
            action(*args)

    def plan(self, order):
        stages, slot, arrivals = [], 0, []
        place = dict(self.home)
        relay = []
        for axis in order:
            last = axis == order[2]
            shift = lambda d, p=place, a=axis: {
                **p, a: lax.rem(p[a] + d, 2 if a == "z" else 4)
            }
            plus, minus = axis + "+", axis + "-"
            own = place
            if axis == "z":
                now = list(arrivals)
                now.append((self.send, (slot, own, 1, plus)))
                now.append((self.send, (slot + 1, own, 2, minus)))
                other = shift(1)
                arrivals = [
                    (self.arrived, (slot, other, 1, minus)),
                    (self.arrived, (slot + 1, other, 2, plus)),
                ]
                slot += 2
                if last:
                    now.append((self.send, (10, own, 0, "core")))
                stages.append(now)
                if last:
                    stages.append(arrivals + [(self.send, (11, other, 0, "core"))])
                    relay = [(10, own), (11, other)]
            else:
                now = list(arrivals)
                now.append((self.send, (slot, own, 0, plus)))
                now.append((self.send, (slot + 1, own, 0, minus)))
                if last:
                    now.append((self.send, (10, own, 0, "core")))
                stages.append(now)
                before, after, far = shift(3), shift(1), shift(2)
                now = [
                    (self.arrived, (slot, before, 0, minus)),
                    (self.send, (slot + 2, before, 1, plus)),
                    (self.arrived, (slot + 1, after, 0, plus)),
                    (self.send, (slot + 3, after, 2, minus)),
                ]
                if last:
                    now.append((self.send, (11, before, 0, "core")))
                    now.append((self.send, (12, after, 0, "core")))
                stages.append(now)
                arrivals = [
                    (self.arrived, (slot + 2, far, 1, minus)),
                    (self.arrived, (slot + 3, far, 2, plus)),
                ]
                if last:
                    stages.append(arrivals + [(self.send, (13, far, 0, "core"))])
                    relay = [(10, own), (11, before), (12, after), (13, far)]
                slot += 4
            place = {**place, axis: None}
        stages.append([(self.arrived, (n, p, 0, "core")) for n, p in relay])
        return stages


def rms_rows(source, gain, target, rows):
    values = source[rows, :].astype(F32)
    scale = lax.rsqrt(jnp.mean(values * values, axis=-1, keepdims=True) + 1e-06)
    target[rows, :] = (values * scale * gain[...].astype(F32)).astype(BF16)


def dot(a, b):
    return jnp.dot(a, b, preferred_element_type=F32)


def dot_nt(a, b):
    return lax.dot_general(a, b, (((1,), (1,)), ((), ())), preferred_element_type=F32)


def kernel(
    tokens,
    shard,
    norm_mix,
    spatial,
    bias,
    gain,
    shift,
    norm_ffn,
    out,
    buf,
    rows_in,
    normed,
    pre,
    gated,
    hmid,
    hidden,
    acc,
    staged,
    send_sems,
    recv_sems,
    local_sems,
    out_sems,
):
    r, f, t = lax.axis_index("rep"), lax.axis_index("fs"), lax.axis_index("tp")
    z, y, x = f // 16, lax.rem(f // 4, 4), lax.rem(f, 4)
    up, down = lax.rem(2 * r + z + 1, 4), lax.rem(2 * r + z + 3, 4)
    at = lambda zz, yy, xx, tt: (zz // 2, lax.rem(zz, 2) * 16 + yy * 4 + xx, tt)
    here = 2 * r + z
    to = {
        "x+": at(here, y, lax.rem(x + 1, 4), t),
        "x-": at(here, y, lax.rem(x + 3, 4), t),
        "y+": at(here, lax.rem(y + 1, 4), x, t),
        "y-": at(here, lax.rem(y + 3, 4), x, t),
        "z+": at(up, y, x, t),
        "z-": at(down, y, x, t),
        "core": at(here, y, x, 1 - t),
    }

    own = pltpu.make_async_copy(shard, buf.at[t, z, y, x], local_sems.at[0])
    own.start()
    count = rows_in.shape[0]
    load = pltpu.make_async_copy(
        tokens.at[pl.ds(t * count, count)], rows_in, local_sems.at[1]
    )
    load.start()

    barrier = pltpu.get_barrier_semaphore()
    for device in to.values():
        pl.semaphore_signal(barrier, inc=1, device_id=device, device_id_type=MESH)
    pl.semaphore_wait(barrier, len(to))
    own.wait()

    where = (t, {"z": z, "y": y, "x": x}, to)
    flows = [Flow(i, buf, send_sems, recv_sems, where) for i in range(len(FLOWS))]

    blocks = count // LANES

    def over_rows(body):
        def step(i, carry):
            body(pl.ds(pl.multiple_of(i * LANES, LANES), LANES))
            return carry

        lax.fori_loop(0, blocks, step, 0)

    def columns(tt, first, size):
        return buf[tt, :, :, :, :, pl.ds(first, size)].reshape(2048, size)

    def spatial_group(g):
        tt, low = g // 2, (g % 2) * 256
        pre[:, 0:256] = dot(normed[...], columns(tt, UNIT + low, 256))
        pre[:, 256:512] = dot(normed[...], columns(tt, VALUE + low, 256))
        at_row = lax.broadcasted_iota(jnp.int32, (128, 128), 0)
        at_col = lax.broadcasted_iota(jnp.int32, (128, 128), 1)
        weights = jnp.where(at_row >= at_col, spatial[g], jnp.zeros((128, 128), BF16))
        g_gain = gain[:, g * 256 : g * 256 + 256].astype(F32)
        g_shift = shift[:, g * 256 : g * 256 + 256].astype(F32)

        def body(rows):
            active = jax.nn.gelu(pre[rows, 256:512], approximate=True)
            center = jnp.mean(active, axis=-1, keepdims=True)
            off = active - center
            spread = jnp.mean(off * off, axis=-1, keepdims=True)
            grouped = off * lax.rsqrt(spread + 1e-06) * g_gain + g_shift
            mixed = dot(weights, grouped.astype(BF16)) + bias[g]
            value = jax.nn.gelu(pre[rows, 0:256], approximate=True) * mixed
            gated[rows, g * 256 : g * 256 + 256] = value.astype(BF16)

        over_rows(body)

    def mix_out(block, carry):
        zz, yy = block // 4, lax.rem(block, 4)
        cols = pl.ds(pl.multiple_of(block * 256, 256), 256)
        total = rows_in[:, cols].astype(F32)
        for tt in range(2):
            w = buf[tt, zz, yy, :, :, pl.ds(MIX, 512)].reshape(256, 512)
            total = total + dot_nt(gated[:, tt * 512 : tt * 512 + 512], w)
        hmid[:, cols] = total.astype(BF16)
        return carry

    def gate_up(tt, pair, pairs):
        def step(i, carry):
            first = pl.multiple_of(PAIRS + i * 256, 256)
            both = dot(normed[...], columns(tt, first, 256))
            value = jax.nn.silu(both[:, 0:128]) * both[:, 128:256]
            into = pl.ds(pl.multiple_of(tt * HALF_FF + i * 128, 128), 128)
            hidden[:, into] = value.astype(BF16)
            return carry

        lax.fori_loop(pair, pair + pairs, step, 0)

    def out_copy(block):
        cols = pl.ds(pl.multiple_of(block * 256, 256), 256)
        return pltpu.make_async_copy(staged.at[block], out.at[:, cols], out_sems.at[block])

    def project_down(part):
        first, size = DOWN_PARTS[part]

        def step(block, carry):
            zz, yy = block // 4, lax.rem(block, 4)
            cols = pl.ds(pl.multiple_of(block * 256, 256), 256)
            total = acc[block] if part else hmid[:, cols].astype(F32)
            for tt in range(2):
                w = buf[tt, zz, yy, :, :, pl.ds(DOWN + first, size)].reshape(256, size)
                a = hidden[:, tt * HALF_FF + first : tt * HALF_FF + first + size]
                total = total + dot_nt(a, w)
            if part == len(DOWN_PARTS) - 1:
                staged[block] = total.astype(BF16)
                out_copy(block).start()
            else:
                acc[block] = total
            return carry

        return step

    def run(op, *args):
        if op == "s":
            flows[args[0]].stage(args[1])
        elif op == "n1":
            load.wait()
            over_rows(functools.partial(rms_rows, rows_in, norm_mix, normed))
        elif op == "n2":
            over_rows(functools.partial(rms_rows, hmid, norm_ffn, normed))
        elif op == "g":
            spatial_group(args[0])
        elif op == "m":
            lax.fori_loop(args[0], args[1], mix_out, 0)
        elif op == "u":
            gate_up(lax.rem(t + args[0], 2), args[1], args[2])
        else:
            lax.fori_loop(args[1], args[2], project_down(args[0]), 0)

    for item in SCHEDULE:
        run(*item)
    for block in range(8):
        out_copy(block).wait()
    for flow in flows:
        for copy in flow.sent:
            copy.wait_send()


def on_device(
    tokens,
    norm_mix,
    w_unit,
    w_value,
    spatial,
    spatial_bias,
    group_gain,
    group_shift,
    w_mix_out,
    norm_ffn,
    w_gate,
    w_up,
    w_down,
):
    count, width = tokens.shape
    half = count // 2
    pairs = jnp.stack([w_gate.reshape(64, 11, 128), w_up.reshape(64, 11, 128)], axis=2)
    shard = jnp.concatenate(
        [w_unit, w_value, w_mix_out.T, pairs.reshape(64, 2816), w_down.T], axis=1
    )
    any_space = pl.BlockSpec(memory_space=pl.ANY)
    vmem = pl.BlockSpec(memory_space=pltpu.VMEM)
    return pl.pallas_call(
        kernel,
        out_shape=jax.ShapeDtypeStruct((half, width), BF16),
        in_specs=[any_space, any_space] + [vmem] * 6,
        out_specs=any_space,
        scratch_shapes=[
            pltpu.VMEM((2, 2, 4, 4, 64, WIDTH), BF16),
            pltpu.VMEM((half, width), BF16),
            pltpu.VMEM((half, width), BF16),
            pltpu.VMEM((half, 512), F32),
            pltpu.VMEM((half, 1024), BF16),
            pltpu.VMEM((half, width), BF16),
            pltpu.VMEM((half, 2 * HALF_FF), BF16),
            pltpu.VMEM((8, half, 256), F32),
            pltpu.VMEM((8, half, 256), BF16),
            pltpu.SemaphoreType.DMA((len(FLOWS), SENDS)),
            pltpu.SemaphoreType.DMA((len(FLOWS), SENDS)),
            pltpu.SemaphoreType.DMA((2,)),
            pltpu.SemaphoreType.DMA((8,)),
        ],
        compiler_params=pltpu.CompilerParams(
            collective_id=0, has_side_effects=True, vmem_limit_bytes=67043328
        ),
    )(
        tokens,
        shard,
        norm_mix.reshape(1, -1),
        spatial,
        spatial_bias.astype(F32)[:, :, None],
        group_gain.reshape(1, -1),
        group_shift.reshape(1, -1),
        norm_ffn.reshape(1, -1),
    )


def solution(mesh):
    placed = (
        P(("rep", "fs"), None),
        P(),
        P("fs", "tp"),
        P("fs", "tp"),
        P(),
        P(),
        P(),
        P(),
        P("tp", "fs"),
        P(),
        P("fs", "tp"),
        P("fs", "tp"),
        P("tp", "fs"),
    )
    return jax.shard_map(
        on_device,
        mesh=mesh,
        in_specs=placed,
        out_specs=P(("rep", "fs", "tp"), None),
        check_vma=False,
    )
```

```python
import functools

import jax
import jax.numpy as jnp
from jax import lax
from jax.experimental import pallas as pl
from jax.experimental.pallas import tpu as pltpu
from jax.sharding import PartitionSpec as P

MESH = pl.DeviceIdType.MESH
F32 = jnp.float32
BF16 = jnp.bfloat16
LANES = 128

MIX, PAIRS, DOWN = 1024, 1536, 4352
WIDTH = 5760
HALF_FF = 1408

FLOWS = (
    (0, 2, "yzx"),
    (2, 2, "yxz"),
    (4, 1, "yzx"),
    (5, 3, "xyz"),
    (8, 1, "yxz"),
    (9, 3, "yxz"),
    (12, 4, "xzy"),
    (16, 6, "xzy"),
    (22, 6, "yxz"),
    (28, 4, "xzy"),
    (32, 2, "xyz"),
    (34, 4, "yzx"),
    (38, 4, "yxz"),
    (42, 3, "yzx"),
)
DOWN_PARTS = (
    (0, 512),
    (512, 512),
    (1024, 384),
)
SCHEDULE = (
    ("s", 3, 0),
    ("s", 5, 0),
    ("s", 7, 0),
    ("s", 1, 0),
    ("s", 2, 0),
    ("s", 0, 0),
    ("n1",),
    ("s", 6, 0),
    ("s", 3, 1),
    ("s", 5, 1),
    ("s", 4, 0),
    ("s", 1, 1),
    ("s", 2, 1),
    ("s", 0, 1),
    ("s", 8, 0),
    ("s", 7, 1),
    ("s", 5, 2),
    ("s", 4, 1),
    ("s", 1, 2),
    ("s", 2, 2),
    ("s", 6, 1),
    ("s", 10, 0),
    ("s", 3, 2),
    ("s", 0, 2),
    ("s", 7, 2),
    ("s", 2, 3),
    ("s", 8, 1),
    ("s", 4, 2),
    ("s", 0, 3),
    ("s", 5, 3),
    ("s", 9, 0),
    ("s", 11, 0),
    ("s", 12, 0),
    ("s", 3, 3),
    ("s", 8, 2),
    ("s", 7, 3),
    ("s", 1, 3),
    ("s", 6, 2),
    ("s", 11, 1),
    ("s", 10, 1),
    ("s", 13, 0),
    ("s", 12, 1),
    ("s", 2, 4),
    ("s", 3, 4),
    ("s", 6, 3),
    ("s", 4, 3),
    ("s", 0, 4),
    ("s", 5, 4),
    ("s", 3, 5),
    ("s", 3, 6),
    ("s", 9, 1),
    ("s", 3, 7),
    ("s", 7, 4),
    ("s", 11, 2),
    ("s", 13, 1),
    ("s", 8, 3),
    ("s", 5, 5),
    ("s", 5, 6),
    ("s", 12, 2),
    ("s", 1, 4),
    ("s", 10, 2),
    ("s", 2, 5),
    ("s", 11, 3),
    ("s", 4, 4),
    ("s", 5, 7),
    ("s", 2, 7),
    ("g", 1),
    ("s", 9, 2),
    ("s", 1, 5),
    ("s", 1, 6),
    ("s", 0, 5),
    ("g", 3),
    ("s", 6, 4),
    ("s", 1, 7),
    ("s", 4, 5),
    ("s", 8, 4),
    ("s", 4, 6),
    ("s", 0, 7),
    ("g", 0),
    ("s", 9, 3),
    ("g", 2),
    ("s", 12, 3),
    ("s", 4, 7),
    ("m", 0, 0, 4),
    ("s", 7, 5),
    ("m", 1, 0, 2),
    ("s", 13, 2),
    ("m", 1, 2, 4),
    ("n2",),
    ("s", 10, 3),
    ("s", 7, 7),
    ("u", 0, 2, 2),
    ("u", 1, 2, 2),
    ("s", 11, 4),
    ("s", 6, 5),
    ("u", 0, 0, 2),
    ("s", 12, 4),
    ("s", 8, 5),
    ("s", 8, 6),
    ("u", 0, 4, 2),
    ("u", 0, 6, 2),
    ("s", 6, 7),
    ("s", 13, 3),
    ("u", 1, 0, 2),
    ("s", 11, 5),
    ("s", 8, 7),
    ("u", 1, 4, 2),
    ("s", 9, 4),
    ("u", 1, 6, 2),
    ("s", 10, 4),
    ("s", 11, 7),
    ("d", 0, 0, 0, 4),
    ("d", 0, 1, 0, 2),
    ("s", 12, 5),
    ("s", 12, 6),
    ("s", 13, 4),
    ("d", 0, 1, 2, 4),
    ("d", 1, 0, 0, 4),
    ("s", 9, 5),
    ("s", 12, 7),
    ("d", 1, 1, 0, 4),
    ("s", 10, 5),
    ("s", 10, 6),
    ("u", 0, 8, 3),
    ("s", 9, 7),
    ("s", 13, 5),
    ("s", 10, 7),
    ("u", 1, 8, 3),
    ("s", 13, 7),
    ("d", 2, 0, 0, 4),
    ("d", 2, 1, 0, 4),
)
class Flow:
    def __init__(self, index, buf, send_sems, recv_sems, where):
        first, tiles, order = FLOWS[index]
        self.index = index
        self.cols = pl.ds(first * LANES, tiles * LANES)
        self.buf, self.send_sems, self.recv_sems = buf, send_sems, recv_sems
        self.core, self.home, self.to = where
        self.sent = []
        self.stages = self.plan(order)

    def part(self, place, rows, core):
        row = (pl.ds(0, 64), pl.ds(0, 32), pl.ds(32, 32))[rows]
        at = [slice(None) if place[a] is None else place[a] for a in "zyx"]
        return self.buf.at[core, at[0], at[1], at[2], row, self.cols]

    def copy(self, sems, ref, device):
        return pltpu.make_async_remote_copy(
            src_ref=ref,
            dst_ref=ref,
            send_sem=self.send_sems.at[self.index, sems[0]],
            recv_sem=self.recv_sems.at[self.index, sems[1]],
            device_id=self.to[device],
            device_id_type=MESH,
        )

    def send(self, sems, place, rows, device):
        self.copy(sems, self.part(place, rows, self.core), device).start()

    def arrived(self, sems, place, core=0):
        core = 1 - self.core if core else self.core
        self.copy(sems, self.part(place, 0, core), "core").wait_recv()

    def finish(self):
        for sem, place in self.sent:
            self.copy((sem, 0), self.part(place, 0, self.core), "core").wait_send()

    def stage(self, number):
        for action, *args in self.stages[number]:
            action(*args)

    def plan(self, order):
        send, arrived = self.send, self.arrived
        stages, recv, arrivals = [], 0, []
        place = dict(self.home)
        every = dict.fromkeys("zyx")
        for phase, axis in enumerate(order):
            last = phase == 2
            put = lambda v, p=place, a=axis: {**p, a: v}
            shift = lambda d, p=place, a=axis: put(lax.rem(p[a] + d, 2 if a == "z" else 4))
            plus, minus = axis + "+", axis + "-"
            one, two, relay = (phase, recv), (phase, recv + 1), (3, 5)
            if axis == "z":
                recv += 1
                other = shift(1)
                now = arrivals + [(send, one, place, 1, plus), (send, one, place, 2, minus)]
                arrivals = [(arrived, one, other)]
                self.sent.append((phase, place))
                if last:
                    now.append((send, relay, place, 0, "core"))
                    after = arrivals + [(send, (3, 6), other, 0, "core")]
                    stages += [now, after]
                    stages.append([(arrived, relay, place, 1)])
                    stages.append([(arrived, (3, 6), other, 1)])
                else:
                    stages.append(now)
            else:
                recv += 2
                now = arrivals + [(send, one, place, 0, plus), (send, one, place, 0, minus)]
                before, after, far = shift(3), shift(1), shift(2)
                then = [
                    (arrived, one, put(pl.ds(0, 2))),
                    (send, two, before, 1, plus),
                    (send, two, after, 2, minus),
                ]
                arrivals = [(arrived, two, far)]
                self.sent.append((phase, put(pl.ds(0, 3))))
                stages += [now, then]
                if last:
                    now.append((send, relay, place, 0, "core"))
                    then.append((send, relay, before, 0, "core"))
                    then.append((send, relay, after, 0, "core"))
                    stages.append(arrivals + [(send, relay, far, 0, "core")])
                    stages.append([])
                    stages.append([(arrived, relay, every, 1)])
            place = {**place, axis: None}
        self.sent.append((3, every))
        return stages


def rms_rows(source, gain, target, rows):
    values = source[rows, :].astype(F32)
    scale = lax.rsqrt(jnp.mean(values * values, axis=-1, keepdims=True) + 1e-06)
    target[rows, :] = (values * scale * gain[...].astype(F32)[None, :]).astype(BF16)


def dot(a, b):
    return jnp.dot(a, b, preferred_element_type=F32)


def dot_nt(a, b):
    return lax.dot_general(a, b, (((1,), (1,)), ((), ())), preferred_element_type=F32)


def kernel(
    tokens,
    w_unit,
    w_value,
    mix_rows,
    w_gate,
    w_up,
    down_rows,
    norm_mix_in,
    spatial_in,
    bias_in,
    gain_in,
    shift_in,
    norm_ffn_in,
    out,
    buf,
    rows_in,
    normed,
    pre,
    gated,
    hidden,
    acc,
    send_sems,
    recv_sems,
    norm_mix,
    spatial,
    bias,
    gain,
    shift,
    norm_ffn,
    local_sems,
):
    r, f, t = lax.axis_index("rep"), lax.axis_index("fs"), lax.axis_index("tp")
    z, y, x = f // 16, lax.rem(f // 4, 4), lax.rem(f, 4)
    up, down = lax.rem(2 * r + z + 1, 4), lax.rem(2 * r + z + 3, 4)
    at = lambda zz, yy, xx, tt: (zz // 2, lax.rem(zz, 2) * 16 + yy * 4 + xx, tt)
    here = 2 * r + z
    to = {
        "x+": at(here, y, lax.rem(x + 1, 4), t),
        "x-": at(here, y, lax.rem(x + 3, 4), t),
        "y+": at(here, lax.rem(y + 1, 4), x, t),
        "y-": at(here, lax.rem(y + 3, 4), x, t),
        "z+": at(up, y, x, t),
        "z-": at(down, y, x, t),
        "core": at(here, y, x, 1 - t),
    }

    barrier = pltpu.get_barrier_semaphore()
    for device in to.values():
        pl.semaphore_signal(barrier, inc=1, device_id=device, device_id_type=MESH)

    mine = buf.at[t, z, y, x]

    def load_own(source, first, size, slot):
        place = mine.at[:, pl.ds(first, size)]
        pltpu.make_async_copy(source, place, local_sems.at[slot]).start()

    for low in range(0, 512, 256):
        half = pl.ds(low, 256)
        load_own(w_unit.at[:, half], 2 * low, 256, 0)
        load_own(w_value.at[:, half], 2 * low + 256, 256, 0)
    load_own(mix_rows, MIX, 512, 0)
    for i in range(HALF_FF // LANES):
        for source, first in ((w_gate, PAIRS), (w_up, PAIRS + LANES)):
            load_own(source.at[:, pl.ds(i * LANES, LANES)], first + 2 * i * LANES, LANES, 2)
    load_own(down_rows, DOWN, HALF_FF, 2)

    def own_ready(first, size, slot):
        place = mine.at[:, pl.ds(first, size)]
        pltpu.make_async_copy(place, place, local_sems.at[slot]).wait()

    count = rows_in.shape[0]
    load = pltpu.make_async_copy(
        tokens.at[pl.ds(t * count, count)], rows_in, local_sems.at[1]
    )
    load.start()
    small = [
        pltpu.make_async_copy(source, target, local_sems.at[3 + i])
        for i, (source, target) in enumerate(
            (
                (norm_mix_in, norm_mix),
                (spatial_in, spatial),
                (bias_in, bias),
                (gain_in, gain),
                (shift_in, shift),
                (norm_ffn_in, norm_ffn),
            )
        )
    ]
    for copy in small:
        copy.start()

    pl.semaphore_wait(barrier, len(to))
    own_ready(0, PAIRS, 0)
    own_ready(PAIRS, WIDTH - PAIRS, 2)

    where = (t, {"z": z, "y": y, "x": x}, to)
    flows = [Flow(i, buf, send_sems, recv_sems, where) for i in range(len(FLOWS))]

    blocks = count // LANES

    def over_rows(body):
        def step(i, carry):
            body(pl.ds(pl.multiple_of(i * LANES, LANES), LANES))
            return carry

        lax.fori_loop(0, blocks, step, 0)

    def columns(tt, first, size):
        return buf[tt, :, :, :, :, pl.ds(first, size)].reshape(2048, size)

    def spatial_group(g):
        tt, low = g // 2, (g % 2) * 256
        pre[...] = dot(normed[...], columns(tt, 2 * low, 512))
        at_row = lax.broadcasted_iota(jnp.int32, (128, 128), 0)
        at_col = lax.broadcasted_iota(jnp.int32, (128, 128), 1)
        weights = jnp.where(at_row >= at_col, spatial[g], jnp.zeros((128, 128), BF16))
        lift = jnp.transpose(jnp.broadcast_to(bias[g : g + 1, :].astype(F32), (128, 128)))
        lift = jnp.concatenate([lift, lift], axis=1)
        g_gain = gain[pl.ds(g * 256, 256)].astype(F32)[None, :]
        g_shift = shift[pl.ds(g * 256, 256)].astype(F32)[None, :]

        def body(rows):
            active = jax.nn.gelu(pre[rows, 256:512], approximate=True)
            center = jnp.mean(active, axis=-1, keepdims=True)
            off = active - center
            spread = jnp.mean(off * off, axis=-1, keepdims=True)
            grouped = off * lax.rsqrt(spread + 1e-06) * g_gain + g_shift
            mixed = dot(weights, grouped.astype(BF16)) + lift
            value = jax.nn.gelu(pre[rows, 0:256], approximate=True) * mixed
            gated[rows, g * 256 : g * 256 + 256] = value.astype(BF16)

        over_rows(body)

    def mix_out(zz, yy):
        block = zz * 4 + yy
        cols = pl.ds(pl.multiple_of(block * 256, 256), 256)
        total = rows_in[:, cols].astype(F32)
        for tt in range(2):
            w = buf[tt, zz, yy, :, :, pl.ds(MIX, 512)].reshape(256, 512)
            total = total + dot_nt(gated[:, tt * 512 : tt * 512 + 512], w)
        rows_in[:, cols] = total.astype(BF16)

    def gate_up(tt, pair, pairs):
        def step(i, carry):
            first = pl.multiple_of(PAIRS + i * 256, 256)
            both = dot(normed[...], columns(tt, first, 256))
            value = jax.nn.silu(both[:, 0:128]) * both[:, 128:256]
            into = pl.ds(pl.multiple_of(tt * HALF_FF + i * 128, 128), 128)
            hidden[:, into] = value.astype(BF16)
            return carry

        lax.fori_loop(pair, pair + pairs, step, 0)

    def project_down(part, zz, yy):
        first, size = DOWN_PARTS[part]
        block = zz * 4 + yy
        cols = pl.ds(pl.multiple_of(block * 256, 256), 256)
        total = acc[block] if part else rows_in[:, cols].astype(F32)
        for tt in range(2):
            w = buf[tt, zz, yy, :, :, pl.ds(DOWN + first, size)].reshape(256, size)
            a = hidden[:, tt * HALF_FF + first : tt * HALF_FF + first + size]
            total = total + dot_nt(a, w)
        if part == len(DOWN_PARTS) - 1:
            out[:, cols] = total.astype(BF16)
        else:
            acc[block] = total

    def over_blocks(body, plane, first, end):
        zz = lax.rem(z + plane, 2)

        def step(yy, carry):
            body(zz, yy)
            return carry

        lax.fori_loop(first, end, step, 0)

    def run(op, *args):
        if op == "s":
            flows[args[0]].stage(args[1])
        elif op == "n1":
            load.wait()
            for copy in small:
                copy.wait()
            over_rows(functools.partial(rms_rows, rows_in, norm_mix, normed))
        elif op == "n2":
            over_rows(functools.partial(rms_rows, rows_in, norm_ffn, normed))
        elif op == "g":
            spatial_group(args[0])
        elif op == "m":
            over_blocks(mix_out, *args)
        elif op == "u":
            gate_up(lax.rem(t + args[0], 2), args[1], args[2])
        else:
            over_blocks(functools.partial(project_down, args[0]), *args[1:])

    for item in SCHEDULE:
        run(*item)
    for flow in flows:
        flow.finish()


def on_device(
    tokens,
    norm_mix,
    w_unit,
    w_value,
    spatial,
    spatial_bias,
    group_gain,
    group_shift,
    w_mix_out,
    norm_ffn,
    w_gate,
    w_up,
    w_down,
):
    count, width = tokens.shape
    half = count // 2
    any_space = pl.BlockSpec(memory_space=pl.ANY)
    vmem = pl.BlockSpec(memory_space=pltpu.VMEM)
    return pl.pallas_call(
        kernel,
        out_shape=pltpu.VMEM((half, width), BF16),
        in_specs=[any_space] * 13,
        out_specs=vmem,
        scratch_shapes=[
            pltpu.VMEM((2, 2, 4, 4, 64, WIDTH), BF16),
            pltpu.VMEM((half, width), BF16),
            pltpu.VMEM((half, width), BF16),
            pltpu.VMEM((half, 512), F32),
            pltpu.VMEM((half, 1024), BF16),
            pltpu.VMEM((half, 2 * HALF_FF), BF16),
            pltpu.VMEM((8, half, 256), F32),
            pltpu.SemaphoreType.DMA((len(FLOWS), 4)),
            pltpu.SemaphoreType.DMA((len(FLOWS), 7)),
            pltpu.VMEM(norm_mix.shape, BF16),
            pltpu.VMEM(spatial.shape, BF16),
            pltpu.VMEM(spatial_bias.shape, BF16),
            pltpu.VMEM(group_gain.shape, BF16),
            pltpu.VMEM(group_shift.shape, BF16),
            pltpu.VMEM(norm_ffn.shape, BF16),
            pltpu.SemaphoreType.DMA((9,)),
        ],
        compiler_params=pltpu.CompilerParams(
            collective_id=0, has_side_effects=True, vmem_limit_bytes=64000000
        ),
    )(
        tokens,
        w_unit,
        w_value,
        w_mix_out.T,
        w_gate,
        w_up,
        w_down.T,
        norm_mix,
        spatial,
        spatial_bias,
        group_gain,
        group_shift,
        norm_ffn,
    )


def solution(mesh):
    placed = (
        P(("rep", "fs"), None),
        P(),
        P("fs", "tp"),
        P("fs", "tp"),
        P(),
        P(),
        P(),
        P(),
        P("tp", "fs"),
        P(),
        P("fs", "tp"),
        P("fs", "tp"),
        P("tp", "fs"),
    )
    return jax.shard_map(
        on_device,
        mesh=mesh,
        in_specs=placed,
        out_specs=P(("rep", "fs", "tp"), None),
        check_vma=False,
    )
```

```python
import functools

import jax
import jax.numpy as jnp
from jax import lax
from jax.experimental import pallas as pl
from jax.experimental.pallas import tpu as pltpu
from jax.sharding import PartitionSpec as P

MESH = pl.DeviceIdType.MESH
F32 = jnp.float32
BF16 = jnp.bfloat16
LANES = 128

MIX, PAIRS, DOWN = 1024, 1536, 4352
WIDTH = 5760
HALF_FF = 1408

FLOWS = (
    (0, 2, "yxz"),
    (2, 2, "xyz"),
    (4, 1, "yxz"),
    (5, 3, "xyz"),
    (8, 1, "xyz"),
    (9, 3, "yxz"),
    (12, 3, "xzy"),
    (15, 4, "xzy"),
    (19, 4, "yxz"),
    (23, 6, "yzx"),
    (29, 3, "yzx"),
    (32, 2, "yxz"),
    (34, 4, "xzy"),
    (38, 4, "yxz"),
    (42, 3, "xzy"),
)
DOWN_PARTS = (
    (0, 512),
    (512, 512),
    (1024, 384),
)
SCHEDULE = (
    ("s", 3, 0),
    ("s", 2, 0),
    ("s", 1, 0),
    ("s", 9, 0),
    ("s", 6, 0),
    ("s", 0, 0),
    ("n1",),
    ("s", 5, 0),
    ("s", 7, 0),
    ("s", 2, 1),
    ("s", 3, 1),
    ("s", 8, 0),
    ("s", 12, 0),
    ("s", 1, 1),
    ("s", 4, 0),
    ("s", 9, 1),
    ("s", 6, 1),
    ("s", 0, 1),
    ("s", 7, 1),
    ("s", 5, 1),
    ("s", 2, 2),
    ("s", 3, 2),
    ("s", 8, 1),
    ("s", 12, 1),
    ("s", 1, 2),
    ("s", 4, 1),
    ("s", 9, 2),
    ("s", 13, 0),
    ("s", 0, 2),
    ("s", 6, 2),
    ("s", 5, 2),
    ("s", 7, 2),
    ("s", 2, 3),
    ("s", 12, 2),
    ("s", 4, 2),
    ("s", 10, 0),
    ("s", 3, 3),
    ("s", 8, 2),
    ("s", 0, 3),
    ("s", 11, 0),
    ("s", 9, 3),
    ("s", 1, 3),
    ("s", 6, 3),
    ("s", 13, 1),
    ("s", 5, 3),
    ("s", 2, 4),
    ("s", 14, 0),
    ("s", 4, 3),
    ("s", 7, 3),
    ("s", 10, 1),
    ("s", 12, 3),
    ("s", 3, 4),
    ("s", 11, 1),
    ("s", 1, 4),
    ("s", 8, 3),
    ("s", 2, 5),
    ("s", 2, 6),
    ("s", 0, 4),
    ("s", 2, 7),
    ("s", 6, 4),
    ("s", 3, 5),
    ("s", 3, 6),
    ("s", 13, 2),
    ("s", 4, 4),
    ("s", 3, 7),
    ("g", 1),
    ("s", 1, 5),
    ("s", 1, 6),
    ("g", 3),
    ("s", 9, 4),
    ("s", 1, 7),
    ("s", 0, 5),
    ("s", 0, 6),
    ("s", 5, 4),
    ("s", 7, 4),
    ("s", 14, 1),
    ("s", 10, 2),
    ("s", 4, 5),
    ("s", 4, 6),
    ("s", 8, 4),
    ("s", 0, 7),
    ("g", 0),
    ("g", 2),
    ("s", 5, 5),
    ("s", 5, 6),
    ("s", 4, 7),
    ("s", 13, 3),
    ("m", 0, 0, 2),
    ("s", 12, 4),
    ("s", 11, 2),
    ("m", 0, 2, 4),
    ("s", 10, 3),
    ("s", 5, 7),
    ("m", 1, 0, 4),
    ("s", 6, 5),
    ("n2",),
    ("s", 9, 5),
    ("u", 0, 6, 2),
    ("s", 6, 7),
    ("s", 14, 2),
    ("s", 13, 4),
    ("s", 9, 7),
    ("u", 1, 6, 2),
    ("s", 7, 5),
    ("u", 0, 0, 2),
    ("s", 8, 5),
    ("s", 8, 6),
    ("s", 11, 3),
    ("u", 0, 2, 2),
    ("s", 7, 7),
    ("s", 14, 3),
    ("u", 1, 0, 2),
    ("s", 12, 5),
    ("u", 0, 4, 2),
    ("s", 8, 7),
    ("u", 1, 2, 2),
    ("s", 12, 7),
    ("d", 0, 0, 0, 2),
    ("s", 10, 4),
    ("d", 0, 0, 2, 4),
    ("s", 11, 4),
    ("u", 1, 4, 2),
    ("d", 0, 1, 0, 4),
    ("s", 13, 5),
    ("s", 14, 4),
    ("s", 13, 6),
    ("d", 1, 0, 0, 4),
    ("s", 10, 5),
    ("u", 0, 8, 2),
    ("s", 13, 7),
    ("d", 1, 1, 2, 4),
    ("d", 1, 1, 0, 2),
    ("s", 11, 5),
    ("s", 11, 6),
    ("u", 0, 10, 1),
    ("s", 10, 7),
    ("s", 14, 5),
    ("u", 1, 8, 2),
    ("s", 11, 7),
    ("u", 1, 10, 1),
    ("s", 14, 7),
    ("d", 2, 1, 2, 4),
    ("d", 2, 0, 0, 2),
    ("d", 2, 1, 0, 2),
    ("d", 2, 0, 2, 4),
)
class Flow:
    def __init__(self, index, buf, send_sems, recv_sems, where):
        first, tiles, order = FLOWS[index]
        self.index = index
        self.cols = pl.ds(first * LANES, tiles * LANES)
        self.buf, self.send_sems, self.recv_sems = buf, send_sems, recv_sems
        self.core, self.home, self.to = where
        self.sent = []
        self.stages = self.plan(order)

    def part(self, place, rows, core):
        row = (pl.ds(0, 64), pl.ds(0, 32), pl.ds(32, 32))[rows]
        at = [slice(None) if place[a] is None else place[a] for a in "zyx"]
        return self.buf.at[core, at[0], at[1], at[2], row, self.cols]

    def copy(self, sems, ref, device):
        return pltpu.make_async_remote_copy(
            src_ref=ref,
            dst_ref=ref,
            send_sem=self.send_sems.at[self.index, sems[0]],
            recv_sem=self.recv_sems.at[self.index, sems[1]],
            device_id=self.to[device],
            device_id_type=MESH,
        )

    def send(self, sems, place, rows, device):
        self.copy(sems, self.part(place, rows, self.core), device).start()

    def arrived(self, sems, place, core=0):
        core = 1 - self.core if core else self.core
        self.copy(sems, self.part(place, 0, core), "core").wait_recv()

    def finish(self):
        for sem, place in self.sent:
            self.copy((sem, 0), self.part(place, 0, self.core), "core").wait_send()

    def stage(self, number):
        for action, *args in self.stages[number]:
            action(*args)

    def plan(self, order):
        send, arrived = self.send, self.arrived
        stages, recv, arrivals = [], 0, []
        place = dict(self.home)
        every = dict.fromkeys("zyx")
        for phase, axis in enumerate(order):
            last = phase == 2
            put = lambda v, p=place, a=axis: {**p, a: v}
            shift = lambda d, p=place, a=axis: put(lax.rem(p[a] + d, 2 if a == "z" else 4))
            plus, minus = axis + "+", axis + "-"
            one, two, relay = (phase, recv), (phase, recv + 1), (3, 5)
            if axis == "z":
                recv += 1
                other = shift(1)
                now = arrivals + [(send, one, place, 1, plus), (send, one, place, 2, minus)]
                arrivals = [(arrived, one, other)]
                self.sent.append((phase, place))
                if last:
                    now.append((send, relay, place, 0, "core"))
                    after = arrivals + [(send, (3, 6), other, 0, "core")]
                    stages += [now, after]
                    stages.append([(arrived, relay, place, 1)])
                    stages.append([(arrived, (3, 6), other, 1)])
                else:
                    stages.append(now)
            else:
                recv += 2
                now = arrivals + [(send, one, place, 0, plus), (send, one, place, 0, minus)]
                before, after, far = shift(3), shift(1), shift(2)
                then = [
                    (arrived, one, put(pl.ds(0, 2))),
                    (send, two, before, 1, plus),
                    (send, two, after, 2, minus),
                ]
                arrivals = [(arrived, two, far)]
                self.sent.append((phase, put(pl.ds(0, 3))))
                stages += [now, then]
                if last:
                    now.append((send, relay, place, 0, "core"))
                    then.append((send, relay, before, 0, "core"))
                    then.append((send, relay, after, 0, "core"))
                    stages.append(arrivals + [(send, relay, far, 0, "core")])
                    stages.append([])
                    stages.append([(arrived, relay, every, 1)])
            place = {**place, axis: None}
        self.sent.append((3, every))
        return stages


def rms_rows(source, gain, target, rows):
    values = source[rows, :].astype(F32)
    scale = lax.rsqrt(jnp.mean(values * values, axis=-1, keepdims=True) + 1e-06)
    target[rows, :] = (values * scale * gain[...].astype(F32)[None, :]).astype(BF16)


def dot(a, b):
    return jnp.dot(a, b, preferred_element_type=F32)


def dot_nt(a, b):
    return lax.dot_general(a, b, (((1,), (1,)), ((), ())), preferred_element_type=F32)


def kernel(
    tokens,
    w_unit,
    w_value,
    mix_rows,
    w_gate,
    w_up,
    down_rows,
    norm_mix_in,
    spatial_in,
    bias_in,
    gain_in,
    shift_in,
    norm_ffn_in,
    out,
    buf,
    rows_in,
    normed,
    pre,
    gated,
    hidden,
    acc,
    send_sems,
    recv_sems,
    norm_mix,
    spatial,
    bias,
    gain,
    shift,
    norm_ffn,
    local_sems,
):
    r, f, t = lax.axis_index("rep"), lax.axis_index("fs"), lax.axis_index("tp")
    z, y, x = f // 16, lax.rem(f // 4, 4), lax.rem(f, 4)
    up, down = lax.rem(2 * r + z + 1, 4), lax.rem(2 * r + z + 3, 4)
    at = lambda zz, yy, xx, tt: (zz // 2, lax.rem(zz, 2) * 16 + yy * 4 + xx, tt)
    here = 2 * r + z
    to = {
        "x+": at(here, y, lax.rem(x + 1, 4), t),
        "x-": at(here, y, lax.rem(x + 3, 4), t),
        "y+": at(here, lax.rem(y + 1, 4), x, t),
        "y-": at(here, lax.rem(y + 3, 4), x, t),
        "z+": at(up, y, x, t),
        "z-": at(down, y, x, t),
        "core": at(here, y, x, 1 - t),
    }

    barrier = pltpu.get_barrier_semaphore()
    for device in to.values():
        pl.semaphore_signal(barrier, inc=1, device_id=device, device_id_type=MESH)

    mine = buf.at[t, z, y, x]

    def load_own(source, first, size, slot):
        place = mine.at[:, pl.ds(first, size)]
        pltpu.make_async_copy(source, place, local_sems.at[slot]).start()

    for low in range(0, 512, 256):
        half = pl.ds(low, 256)
        load_own(w_unit.at[:, half], 2 * low, 256, 0)
        load_own(w_value.at[:, half], 2 * low + 256, 256, 0)
    load_own(mix_rows, MIX, 512, 0)
    for i in range(HALF_FF // LANES):
        for source, first in ((w_gate, PAIRS), (w_up, PAIRS + LANES)):
            load_own(source.at[:, pl.ds(i * LANES, LANES)], first + 2 * i * LANES, LANES, 2)
    load_own(down_rows, DOWN, HALF_FF, 2)

    def own_ready(first, size, slot):
        place = mine.at[:, pl.ds(first, size)]
        pltpu.make_async_copy(place, place, local_sems.at[slot]).wait()

    count = rows_in.shape[0]
    load = pltpu.make_async_copy(
        tokens.at[pl.ds(t * count, count)], rows_in, local_sems.at[1]
    )
    load.start()
    small = [
        pltpu.make_async_copy(source, target, local_sems.at[3 + i])
        for i, (source, target) in enumerate(
            (
                (norm_mix_in, norm_mix),
                (spatial_in, spatial),
                (bias_in, bias),
                (gain_in, gain),
                (shift_in, shift),
                (norm_ffn_in, norm_ffn),
            )
        )
    ]
    for copy in small:
        copy.start()

    pl.semaphore_wait(barrier, len(to))
    own_ready(0, PAIRS, 0)
    own_ready(PAIRS, WIDTH - PAIRS, 2)

    where = (t, {"z": z, "y": y, "x": x}, to)
    flows = [Flow(i, buf, send_sems, recv_sems, where) for i in range(len(FLOWS))]

    blocks = count // LANES

    def over_rows(body):
        for i in range(blocks):
            body(pl.ds(i * LANES, LANES))

    def columns(tt, first, size):
        return buf[tt, :, :, :, :, pl.ds(first, size)].reshape(2048, size)

    def spatial_group(g):
        tt, low = g // 2, (g % 2) * 256
        pre[...] = dot(normed[...], columns(tt, 2 * low, 512))
        at_row = lax.broadcasted_iota(jnp.int32, (128, 128), 0)
        at_col = lax.broadcasted_iota(jnp.int32, (128, 128), 1)
        weights = jnp.where(at_row >= at_col, spatial[g], jnp.zeros((128, 128), BF16))
        lift = jnp.transpose(jnp.broadcast_to(bias[g : g + 1, :].astype(F32), (128, 128)))
        lift = jnp.concatenate([lift, lift], axis=1)
        g_gain = gain[pl.ds(g * 256, 256)].astype(F32)[None, :]
        g_shift = shift[pl.ds(g * 256, 256)].astype(F32)[None, :]

        def body(rows):
            active = jax.nn.gelu(pre[rows, 256:512], approximate=True)
            center = jnp.mean(active, axis=-1, keepdims=True)
            off = active - center
            spread = jnp.mean(off * off, axis=-1, keepdims=True)
            grouped = off * lax.rsqrt(spread + 1e-06) * g_gain + g_shift
            mixed = dot(weights, grouped.astype(BF16)) + lift
            value = jax.nn.gelu(pre[rows, 0:256], approximate=True) * mixed
            gated[rows, g * 256 : g * 256 + 256] = value.astype(BF16)

        over_rows(body)

    def mix_out(zz, yy):
        block = zz * 4 + yy
        cols = pl.ds(pl.multiple_of(block * 256, 256), 256)
        total = rows_in[:, cols].astype(F32)
        for tt in range(2):
            w = buf[tt, zz, yy, :, :, pl.ds(MIX, 512)].reshape(256, 512)
            total = total + dot_nt(gated[:, tt * 512 : tt * 512 + 512], w)
        rows_in[:, cols] = total.astype(BF16)

    def gate_up(tt, pair, pairs):
        for i in range(pair, pair + pairs):
            both = dot(normed[...], columns(tt, PAIRS + i * 256, 256))
            value = jax.nn.silu(both[:, 0:128]) * both[:, 128:256]
            into = pl.ds(pl.multiple_of(tt * HALF_FF + i * 128, 128), 128)
            hidden[:, into] = value.astype(BF16)

    def project_down(part, zz, yy):
        first, size = DOWN_PARTS[part]
        block = zz * 4 + yy
        cols = pl.ds(pl.multiple_of(block * 256, 256), 256)
        total = acc[block] if part else rows_in[:, cols].astype(F32)
        for tt in range(2):
            w = buf[tt, zz, yy, :, :, pl.ds(DOWN + first, size)].reshape(256, size)
            a = hidden[:, tt * HALF_FF + first : tt * HALF_FF + first + size]
            total = total + dot_nt(a, w)
        if part == len(DOWN_PARTS) - 1:
            out[:, cols] = total.astype(BF16)
        else:
            acc[block] = total

    def over_blocks(body, plane, first, end):
        zz = lax.rem(z + plane, 2)

        for yy in range(first, end):
            body(zz, yy)

    def run(op, *args):
        if op == "s":
            flows[args[0]].stage(args[1])
        elif op == "n1":
            load.wait()
            for copy in small:
                copy.wait()
            over_rows(functools.partial(rms_rows, rows_in, norm_mix, normed))
        elif op == "n2":
            over_rows(functools.partial(rms_rows, rows_in, norm_ffn, normed))
        elif op == "g":
            spatial_group(args[0])
        elif op == "m":
            over_blocks(mix_out, *args)
        elif op == "u":
            gate_up(lax.rem(t + args[0], 2), args[1], args[2])
        else:
            over_blocks(functools.partial(project_down, args[0]), *args[1:])

    for item in SCHEDULE:
        run(*item)
    for flow in flows:
        flow.finish()


def on_device(
    tokens,
    norm_mix,
    w_unit,
    w_value,
    spatial,
    spatial_bias,
    group_gain,
    group_shift,
    w_mix_out,
    norm_ffn,
    w_gate,
    w_up,
    w_down,
):
    count, width = tokens.shape
    half = count // 2
    any_space = pl.BlockSpec(memory_space=pl.ANY)
    vmem = pl.BlockSpec(memory_space=pltpu.VMEM)
    return pl.pallas_call(
        kernel,
        out_shape=pltpu.VMEM((half, width), BF16),
        in_specs=[any_space] * 13,
        out_specs=vmem,
        scratch_shapes=[
            pltpu.VMEM((2, 2, 4, 4, 64, WIDTH), BF16),
            pltpu.VMEM((half, width), BF16),
            pltpu.VMEM((half, width), BF16),
            pltpu.VMEM((half, 512), F32),
            pltpu.VMEM((half, 1024), BF16),
            pltpu.VMEM((half, 2 * HALF_FF), BF16),
            pltpu.VMEM((8, half, 256), F32),
            pltpu.SemaphoreType.DMA((len(FLOWS), 4)),
            pltpu.SemaphoreType.DMA((len(FLOWS), 7)),
            pltpu.VMEM(norm_mix.shape, BF16),
            pltpu.VMEM(spatial.shape, BF16),
            pltpu.VMEM(spatial_bias.shape, BF16),
            pltpu.VMEM(group_gain.shape, BF16),
            pltpu.VMEM(group_shift.shape, BF16),
            pltpu.VMEM(norm_ffn.shape, BF16),
            pltpu.SemaphoreType.DMA((9,)),
        ],
        compiler_params=pltpu.CompilerParams(
            collective_id=0, has_side_effects=True, vmem_limit_bytes=64000000
        ),
    )(
        tokens,
        w_unit,
        w_value,
        w_mix_out.T,
        w_gate,
        w_up,
        w_down.T,
        norm_mix,
        spatial,
        spatial_bias,
        group_gain,
        group_shift,
        norm_ffn,
    )


def solution(mesh):
    placed = (
        P(("rep", "fs"), None),
        P(),
        P("fs", "tp"),
        P("fs", "tp"),
        P(),
        P(),
        P(),
        P(),
        P("tp", "fs"),
        P(),
        P("fs", "tp"),
        P("fs", "tp"),
        P("tp", "fs"),
    )
    return jax.shard_map(
        on_device,
        mesh=mesh,
        in_specs=placed,
        out_specs=P(("rep", "fs", "tp"), None),
        check_vma=False,
    )
```
